32 devices in a mesh: sp: 8 (over z, x), tp: 4 (over y, core).
Axes of the slice: x: 2, y: 2, z: 4, core: 2. Of those that a mesh axis runs over, the one named last changes fastest.
Arguments:
- hidden_rows: bfloat16 [1024, 2048], P('sp', 'tp'), may hold values from -6 to 6
- out_cot: bfloat16 [1024, 2048], P('sp', 'tp'), may hold values from -6 to 6
- routes: int32 [1024, 2], P('sp'), may hold values from 0 to 7, all different within a row; in each aligned block of 128 rows (0 to 127, 128 to 255, ...) at most 40 rows name the same one
- route_weight: float32 [1024, 2], P('sp'), may hold values from 0.2 to 2
- gate_w: bfloat16 [8, 2048, 1024], P('sp', None, 'tp'), may hold values from -0.125 to 0.125
- up_w: bfloat16 [8, 2048, 1024], P('sp', None, 'tp'), may hold values from -0.125 to 0.125
- down_w: bfloat16 [8, 1024, 2048], P('sp', 'tp'), may hold values from -0.1875 to 0.1875
- out_weight: bfloat16 [2048, 4096], P('sp', 'tp'), may hold values from -0.09375 to 0.09375
- step_inputs: bfloat16 [1024, 4096], P('sp', 'tp'), may hold values from -6 to 6
- input_map: bfloat16 [1024, 1024], P('sp', 'tp'), may hold values from -2 to 2
- output_map: bfloat16 [1024, 1024], P('sp', 'tp'), may hold values from -2 to 2
- log_decay: float32 [1024, 64], P('sp', 'tp'), may hold values from -1 to 0, as said below
- gate_z: bfloat16 [1024, 4096], P('sp', 'tp'), may hold values from -6 to 6
Outputs:
- grad_gate_w: float32 [8, 2048, 1024], P('sp', None, 'tp')
- grad_up_w: float32 [8, 2048, 1024], P('sp', None, 'tp')
- grad_down_w: float32 [8, 1024, 2048], P('sp', 'tp')
- grad_out_weight: float32 [2048, 4096], P('sp', 'tp')
- grad_step: bfloat16 [1024, 4096], P('sp', 'tp')
- grad_gate_z: bfloat16 [1024, 4096], P('sp', 'tp')
- grad_input_map: float32 [1024, 1024], P('sp', 'tp')
- grad_output_map: float32 [1024, 1024], P('sp', 'tp')
- grad_log_decay: float32 [1024, 64], P('sp', 'tp')
The draws below stay inside these ranges and needn't reach their ends.
Inputs may be any that keep to these rules, and one draw needn't show every extreme that they name: `routes`: each row names 2 different experts. Among the positions of one index of sp no expert is named more than 40 times, a bound that some block reaches. `log_decay`: every entry is negative.
All inputs are finite; a program needn't handle non-finite values.
Results may differ from the reference program's by a relative error of at most 0.015.
Values may be sent and summed in bfloat16 or wider, within the bound.
A program may use at most 128 MiB of HBM per device.

```python
import math
import jax
import jax.numpy as jnp
import numpy as np
from jax import lax

D = 2048
MIXER_HEADS = 64
HEAD_DIM = 64
GROUPS = 8
NS = 128
FF = 1024
TOP = 2
BLOCK = 128
TOK_DEV = 128
SEQUENCE_TOKENS = 1024
EXPERTS = 8
INNER = 4096
CAP = 40
N_SP = 8
N_TP = 4


def draw_log_decay(key, part):
    random_child_keys = jax.random.split(key, 7)
    slow_share = 0.5
    rough_low = 0.5
    rough_high = 1.5
    slow_heads = jax.random.bernoulli(random_child_keys[0], slow_share, (MIXER_HEADS,))
    fast_rate = jnp.exp(jax.random.uniform(random_child_keys[1], (MIXER_HEADS,), jnp.float32, jnp.log(1.0 / 100.0), jnp.log(1.0 / 30.0)))
    slow_rate = jnp.exp(jax.random.uniform(random_child_keys[2], (MIXER_HEADS,), jnp.float32, jnp.log(0.6), jnp.log(1.4))) / SEQUENCE_TOKENS
    head_rate = jnp.where(slow_heads, slow_rate, fast_rate)
    block_factor = jnp.exp(jax.random.uniform(random_child_keys[3], (SEQUENCE_TOKENS // TOK_DEV,), jnp.float32, jnp.log(0.5), jnp.log(2.0)))
    position_factor = jnp.repeat(block_factor, TOK_DEV)
    roughness = jax.random.uniform(random_child_keys[4], (SEQUENCE_TOKENS, MIXER_HEADS), jnp.float32, rough_low, rough_high)
    head_decay_speeds = head_rate[None, :] * position_factor[:, None] * roughness
    spike_position = jax.random.randint(random_child_keys[5], (3,), 0, SEQUENCE_TOKENS)
    spike_retained = jax.random.uniform(random_child_keys[6], (3, MIXER_HEADS), jnp.float32, 0.55, 0.8)
    token_places = jnp.arange(SEQUENCE_TOKENS)
    spike_log_value = jnp.sum(jnp.where(token_places[:, None, None] == spike_position[None, :, None], jnp.log(spike_retained)[None, :, :], 0.0), axis=1)
    return (spike_log_value - head_decay_speeds).astype(jnp.float32)


def strengthened(array, rng, source, target, shards_of, factor):
    owner, partner = [(jnp.arange(array.shape[dim]) // (array.shape[dim] // shards_of)).reshape([-1 if axis == dim else 1 for axis in range(array.ndim)]) for dim in (source, target)]
    chosen = jax.random.permutation(rng, shards_of)[partner]
    strong = (owner == chosen) | (owner == (partner + shards_of // 2) % shards_of)
    return jnp.where(strong, factor * array, array)


def levels(rng, shape, cuts, least, top_value):
    gain, own = 1.0, jax.random.fold_in(rng, 6)
    for axis_at, parts in cuts:
        draws = jnp.exp(jax.random.uniform(jax.random.fold_in(own, axis_at), (parts,), jnp.float32, least / len(cuts), top_value / len(cuts)))
        gain = gain * jnp.repeat(draws, shape[axis_at] // parts).reshape([-1 if axis == axis_at else 1 for axis in range(len(shape))])
    return gain


def deal_out(stream_key, own, number, rows, number_of, top, limit, slope):
    order = jax.random.permutation(stream_key, number_of)
    heavy_load, usual = load_shares(number_of, rows * top, limit, slope, True), load_shares(number_of, rows * top, limit, slope, False)
    places = jnp.arange(number_of)

    def named(lengths, turn):
        used = int((lengths > 0).sum())
        fixed = max(1, used // 4)
        passed = fixed + (places - fixed + turn * (used - fixed)) % max(1, number_of - fixed)
        return jnp.zeros((number_of,), jnp.int32).at[order[jnp.where(places < fixed, places, passed)]].set(jnp.asarray(lengths, jnp.int32))

    lengths = jnp.where(number % 4 == 0, named(heavy_load, number // 4), named(usual, number - number // 4 - 1))
    mixed = jax.random.permutation(jax.random.fold_in(own, 3), number_of)
    source_of, sink = mixed[0:number_of // 2 * 2:2], mixed[1:number_of // 2 * 2:2]
    slack = jnp.minimum(lengths[source_of] - 1, limit - lengths[sink]) // 2
    slack = jnp.where((source_of == order[0]) | (sink == order[0]) | (lengths[sink] == 0), 0, jnp.maximum(slack, 0))
    passed = jax.random.randint(jax.random.fold_in(own, 4), (number_of // 2,), 0, 1 << 20) % (slack + 1)
    lengths = lengths.at[source_of].add(-passed).at[sink].add(passed)
    labels = jnp.searchsorted(jnp.cumsum(lengths), jnp.arange(rows * top), side="right").astype(jnp.int32)
    listing = labels.reshape(top, rows).T
    listing = listing[jax.random.permutation(jax.random.fold_in(own, 1), rows)]
    turn = jax.random.randint(jax.random.fold_in(own, 2), (rows, 1), 0, top)
    return jnp.take_along_axis(listing, (jnp.arange(top)[None, :] + turn) % top, axis=1)


def load_shares(number_of, total, bound, slope, full):
    portions = [(1 << 20) // math.isqrt(grade ** slope) + 1 for grade in range(1, number_of + 1)]
    largest = bound if full else min(bound, max(-(-total // number_of), total * portions[0] // sum(portions)))
    least = 1 if total - largest >= number_of - 1 else 0
    holding, surplus = [largest] + [least] * (number_of - 1), total - largest - least * (number_of - 1)
    while surplus > 0:
        free = [i for i in range(1, number_of) if holding[i] < largest] or [i for i in range(1, number_of) if holding[i] < bound]
        pool, budget = sum([portions[i] for i in free]), surplus
        for i in free:
            extra = min(bound - holding[i], max(1, budget * portions[i] // pool), surplus)
            holding[i] = holding[i] + extra
            surplus = surplus - extra
    return np.array(holding)


def noise(stream_key, shape, deviation, most, shards=(), kind=jnp.bfloat16):
    loudness = levels(stream_key, shape, shards, -0.22, 0.18) if shards else 1.0
    drawn = jax.random.normal(stream_key, shape, jnp.float32) * deviation * loudness
    return jnp.minimum(jnp.maximum(drawn, -most), most).astype(kind)


def heavy_noise(stream_key, dims, width, bound, pieces, heavy, held_as=jnp.bfloat16):
    result = width * jax.random.normal(stream_key, dims, jnp.float32)
    if pieces:
        result = result * levels(stream_key, dims, pieces, -0.22, 0.18)
    return jnp.clip(strengthened(result, jax.random.fold_in(stream_key, 3), *heavy), -bound, bound).astype(held_as)


def setup_inputs(seed: int = 0) -> dict:
    keys = jax.random.split(jax.random.key(seed), 14)
    hidden_rows = noise(keys[0], (SEQUENCE_TOKENS, D), 1.0, 6.0, ((0, 8), (1, 4)))
    out_cot = heavy_noise(keys[1], (SEQUENCE_TOKENS, D), 1.0, 6.0, ((0, 8), (1, 4)), (0, 1, 8, 2.0))
    routes_keys = jax.random.split(jax.random.fold_in(keys[2], 1), SEQUENCE_TOKENS // TOK_DEV)
    routes_turns = jax.random.permutation(jax.random.fold_in(keys[2], 3), SEQUENCE_TOKENS // TOK_DEV)
    routes = jax.vmap(lambda own, number: deal_out(jax.random.fold_in(keys[2], 2), own, number, TOK_DEV, EXPERTS, TOP, CAP, 2))(routes_keys, routes_turns).reshape((SEQUENCE_TOKENS, TOP))
    route_weight = jnp.clip(jnp.exp(math.log(2.0) - 2.3025851 * jax.random.uniform(keys[3], (SEQUENCE_TOKENS, TOP), jnp.float32) ** levels(keys[3], (SEQUENCE_TOKENS, TOP), ((0, 8),), -0.2, 0.2)), 0.2, 2.0)
    gate_w = noise(keys[4], (EXPERTS, D, FF), D ** -0.5, 0.125, ((0, 8), (2, 4)))
    up_w = noise(keys[5], (EXPERTS, D, FF), D ** -0.5, 0.125, ((0, 8), (2, 4)))
    down_w = noise(keys[6], (EXPERTS, FF, D), FF ** -0.5, 0.1875, ((0, 8), (1, 4)))
    out_weight = noise(keys[7], (D, INNER), INNER ** -0.5, 0.09375, ((0, 8), (1, 4)))
    step_inputs = noise(keys[8], (SEQUENCE_TOKENS, INNER), 1.0, 6.0, ((0, 8), (1, 4)))
    input_map = noise(keys[9], (SEQUENCE_TOKENS, GROUPS * NS), 0.3, 2.0, ((0, 8), (1, 4)))
    output_map = noise(keys[10], (SEQUENCE_TOKENS, GROUPS * NS), 0.3, 2.0, ((0, 8), (1, 4)))
    log_decay = draw_log_decay(jax.random.fold_in(keys[13], 71), 0)
    gate_z = noise(keys[12], (SEQUENCE_TOKENS, INNER), 1.0, 6.0, ((0, 8), (1, 4)))
    return dict(hidden_rows=hidden_rows, out_cot=out_cot, routes=routes, route_weight=route_weight, gate_w=gate_w, up_w=up_w, down_w=down_w, out_weight=out_weight, step_inputs=step_inputs, input_map=input_map, output_map=output_map, log_decay=log_decay, gate_z=gate_z)


epsilon = 1e-06
exact_mode = lax.Precision.HIGHEST
by_rows = (((0,), (0,)), ((), ()))
by_cols = (((1,), (1,)), ((), ()))

def block_step(carry_state, inputs):
    x_block, b_block, c_block, log_block = inputs
    per_group = x_block.shape[1] // b_block.shape[1]
    cum_log = jnp.cumsum(log_block, axis=0)
    token_places = jnp.arange(log_block.shape[0])
    lower_mask = (token_places[:, None] >= token_places[None, :])[:, :, None]
    log_spans = jnp.where(lower_mask, cum_log[:, None, :] - cum_log[None, :, :], 0.0)
    decay_mask = jnp.where(lower_mask, jnp.exp(log_spans), 0.0)
    scores = jnp.einsum('tgn,sgn->tsg', c_block, b_block, precision=exact_mode)
    scores = jnp.repeat(scores, per_group, axis=2)
    within = jnp.einsum('tsh,shp->thp', scores * decay_mask, x_block, precision=exact_mode)
    c_heads = jnp.repeat(c_block, per_group, axis=1)
    b_heads = jnp.repeat(b_block, per_group, axis=1)
    carried = jnp.einsum('thn,hpn->thp', c_heads, carry_state, precision=exact_mode) * jnp.exp(cum_log)[:, :, None]
    last_log = cum_log[-1]
    to_end = jnp.exp(last_log[None, :] - cum_log)
    new_state = carry_state * jnp.exp(last_log)[:, None, None] + jnp.einsum('shn,shp->hpn', b_heads * to_end[:, :, None], x_block, precision=exact_mode)
    return (new_state, within + carried)

def mixer_forward(step_in, map_in, map_out, log_in, gate_in, entry_state):
    length, head_count = log_in.shape
    groups = map_in.shape[1] // NS
    blocks = length // BLOCK
    x_blocks = step_in.reshape(blocks, BLOCK, head_count, HEAD_DIM)
    b_blocks = map_in.reshape(blocks, BLOCK, groups, NS)
    c_blocks = map_out.reshape(blocks, BLOCK, groups, NS)
    log_blocks = log_in.reshape(blocks, BLOCK, head_count)
    _, outputs = lax.scan(block_step, entry_state, (x_blocks, b_blocks, c_blocks, log_blocks))
    mixed = outputs.reshape(length, head_count * HEAD_DIM)
    gated = (mixed * jax.nn.silu(gate_in)).reshape(length, groups, -1)
    normed = gated * lax.rsqrt(lax.optimization_barrier(jnp.mean(gated * gated, axis=-1, keepdims=True)) + epsilon)
    return normed.reshape(length, head_count * HEAD_DIM)

def expert_backward(row_block, cot_block, gate_mat, up_mat, down_mat):
    gate_pre = jnp.dot(row_block, gate_mat, preferred_element_type=jnp.float32)
    up_pre = jnp.dot(row_block, up_mat, preferred_element_type=jnp.float32)
    gate_sigmoid = jax.nn.sigmoid(gate_pre)
    hidden = (gate_pre * gate_sigmoid * up_pre).astype(jnp.bfloat16)
    d_act = lax.dot_general(cot_block, down_mat, by_cols, preferred_element_type=jnp.float32)
    d_gate = (d_act * up_pre * gate_sigmoid * (1.0 + gate_pre * (1.0 - gate_sigmoid))).astype(jnp.bfloat16)
    d_up = (d_act * gate_pre * gate_sigmoid).astype(jnp.bfloat16)
    grad_down = lax.dot_general(hidden, cot_block, by_rows, preferred_element_type=jnp.float32)
    grad_gate = lax.dot_general(row_block, d_gate, by_rows, preferred_element_type=jnp.float32)
    grad_up = lax.dot_general(row_block, d_up, by_rows, preferred_element_type=jnp.float32)
    return (grad_gate, grad_up, grad_down, d_gate, d_up)

def reference(hidden_rows, out_cot, routes, route_weight, gate_w, up_w, down_w, out_weight, step_inputs, input_map, output_map, log_decay, gate_z):
    per_source = TOK_DEV * TOP
    buffer_rows = N_SP * CAP
    flat_routes = routes.reshape(N_SP, per_source)
    expert_hits = (flat_routes[:, :, None] == jnp.arange(EXPERTS, dtype=jnp.int32)[None, None, :]).astype(jnp.int32)
    slot_rank = lax.optimization_barrier(jnp.sum((jnp.cumsum(expert_hits, axis=1) - expert_hits) * expert_hits, axis=2))
    source = jnp.arange(N_SP, dtype=jnp.int32)[:, None]
    slot_index = (flat_routes * buffer_rows + source * CAP + slot_rank).reshape(-1).astype(jnp.int32)
    owner_token = jnp.repeat(jnp.arange(SEQUENCE_TOKENS, dtype=jnp.int32), TOP)
    slot_token = jnp.full((EXPERTS * buffer_rows,), SEQUENCE_TOKENS, jnp.int32).at[slot_index].set(owner_token)
    slot_weight = jnp.zeros((EXPERTS * buffer_rows,), jnp.float32).at[slot_index].set(route_weight.reshape(-1))
    padded_rows = jnp.concatenate([hidden_rows, jnp.zeros((1, D), jnp.bfloat16)], axis=0)
    padded_cot = jnp.concatenate([out_cot.astype(jnp.float32), jnp.zeros((1, D), jnp.float32)], axis=0)
    range_width = FF // N_TP

    def per_expert(expert):
        first_slot = (expert * buffer_rows).astype(jnp.int32)
        tokens_here = lax.dynamic_slice_in_dim(slot_token, first_slot, buffer_rows)
        weights_here = lax.dynamic_slice_in_dim(slot_weight, first_slot, buffer_rows)
        row_block = padded_rows[tokens_here]
        cot_block = (padded_cot[tokens_here] * weights_here[:, None]).astype(jnp.bfloat16)
        gate_mat = gate_w[expert]
        up_mat = up_w[expert]
        grad_gate, grad_up, grad_down, d_gate, d_up = expert_backward(row_block, cot_block, gate_mat, up_mat, down_w[expert])
        running = jnp.zeros((buffer_rows, D), jnp.float32)
        for quarter in range(N_TP):
            low_col = quarter * range_width
            high_col = low_col + range_width
            range_term = lax.dot_general(d_gate[:, low_col:high_col], gate_mat[:, low_col:high_col], by_cols, preferred_element_type=jnp.float32)
            range_term = range_term + lax.dot_general(d_up[:, low_col:high_col], up_mat[:, low_col:high_col], by_cols, preferred_element_type=jnp.float32)
            running = running + lax.optimization_barrier(range_term.astype(jnp.bfloat16)).astype(jnp.float32)
        return (grad_gate, grad_up, grad_down, running.astype(jnp.bfloat16))
    grad_gate_w, grad_up_w, grad_down_w, slot_grads = lax.map(per_expert, jnp.arange(EXPERTS, dtype=jnp.int32))
    routed = jax.ops.segment_sum(slot_grads.reshape(-1, D).astype(jnp.float32), slot_token, num_segments=SEQUENCE_TOKENS + 1)[:SEQUENCE_TOKENS]
    mid_grad = (out_cot.astype(jnp.float32) + routed).astype(jnp.bfloat16)
    d_normed = jnp.dot(mid_grad, out_weight, preferred_element_type=jnp.float32)
    start_state = jnp.zeros((MIXER_HEADS, HEAD_DIM, NS), jnp.float32)

    def forward(step_in, map_in, map_out, log_in, gate_in):
        return mixer_forward(step_in, map_in, map_out, log_in, gate_in, start_state)
    normed, pullback = jax.vjp(forward, step_inputs.astype(jnp.float32), input_map.astype(jnp.float32), output_map.astype(jnp.float32), log_decay, gate_z.astype(jnp.float32))
    grad_out_weight = lax.dot_general(mid_grad, normed.astype(jnp.bfloat16), by_rows, preferred_element_type=jnp.float32)
    grad_step, grad_in_map, grad_out_map, grad_log, grad_gate = pullback(d_normed)
    return (grad_gate_w, grad_up_w, grad_down_w, grad_out_weight, grad_step.astype(jnp.bfloat16), grad_gate.astype(jnp.bfloat16), grad_in_map, grad_out_map, grad_log)
```

```python
from functools import partial, reduce

import jax
import jax.numpy as jnp
from jax import lax
from jax.experimental import pallas as pl
from jax.experimental.pallas import tpu as pltpu
from jax.sharding import PartitionSpec as P

D = 2048
HEAD_DIM = 64
NS = 128
TAIL = 16

epsilon = 1e-06
exact_mode = lax.Precision.HIGHEST
f32 = jnp.float32
bf16 = jnp.bfloat16
by_rows = (((0,), (0,)), ((), ()))
by_cols = (((1,), (1,)), ((), ()))


def dot(a, b, dims=(((1,), (0,)), ((), ()))):
    return lax.dot_general(a, b, dims, preferred_element_type=f32)


def exact(a, b, dims=(((1,), (0,)), ((), ()))):
    return lax.dot_general(a, b, dims, precision=exact_mode, preferred_element_type=f32)


def iota(shape, dim):
    return lax.broadcasted_iota(jnp.int32, shape, dim)


def lower(length):
    return iota((length, length), 0) >= iota((length, length), 1)


def spread(heads):
    shape = (heads, heads * HEAD_DIM)
    return (iota(shape, 1) // HEAD_DIM == iota(shape, 0)).astype(f32)


def cum_logs(log):
    return exact(lower(log.shape[0]).astype(f32), log)


def state_kernel(x_ref, b_ref, log_ref, sent_ref, own_ref):
    length, heads = log_ref.shape
    groups = b_ref.shape[1] // NS
    wide = x_ref.shape[1] // groups
    cum = cum_logs(log_ref[...])
    last = cum[length - 1 : length, :]
    to_end = exact(jnp.exp(last - cum), spread(heads))
    weighted = (x_ref[...].astype(f32) * to_end).astype(bf16)
    for g in range(groups):
        state = dot(weighted[:, g * wide : (g + 1) * wide], b_ref[:, g * NS : (g + 1) * NS], by_rows)
        own_ref[g * wide : (g + 1) * wide, :] = state
        sent_ref[g * wide : (g + 1) * wide, :] = state.astype(bf16)
    row = jnp.concatenate([last, jnp.zeros((1, NS - heads), f32)], axis=1)
    high = row.astype(bf16).astype(f32)
    middle = (row - high).astype(bf16).astype(f32)
    low = row - high - middle
    sent_ref[heads * HEAD_DIM :, :] = jnp.concatenate(
        [high, middle, low, jnp.zeros((TAIL - 3, NS), f32)], axis=0
    ).astype(bf16)


def combine(weights_ref, parts_ref, total_ref):
    count, heads = weights_ref.shape

    def one(source, _):
        for h in range(heads):
            rows = slice(h * HEAD_DIM, (h + 1) * HEAD_DIM)
            total_ref[rows, :] += weights_ref[source, h] * parts_ref[source, rows, :].astype(f32)
        return 0

    total_ref[...] = jnp.zeros_like(total_ref)
    lax.fori_loop(0, count, one, 0)


def decay_of(cum, cum_t, mask, h):
    spans = jnp.where(mask, cum[:, h : h + 1] - cum_t[h : h + 1, :], 0.0)
    return jnp.where(mask, jnp.exp(spans), 0.0)


def forward_kernel(
    weights_ref, parts_ref, x_ref, b_ref, c_ref, log_ref, z_ref, entry_ref, y_ref, half_ref
):
    length, heads = log_ref.shape
    groups = b_ref.shape[1] // NS
    wide = x_ref.shape[1] // groups
    per_group = heads // groups
    combine(weights_ref, parts_ref, entry_ref)
    log = log_ref[...]
    mask = lower(length)
    cum = cum_logs(log)
    cum_t = exact(log, mask.astype(f32), (((0,), (1,)), ((), ())))
    grown = exact(jnp.exp(cum), spread(heads))
    for g in range(groups):
        cols = slice(g * wide, (g + 1) * wide)
        c = c_ref[:, g * NS : (g + 1) * NS]
        scores = dot(c, b_ref[:, g * NS : (g + 1) * NS], by_cols)
        carried = dot(c, entry_ref[cols, :].astype(bf16), by_cols) * grown[:, cols]
        within = [
            dot(
                (scores * decay_of(cum, cum_t, mask, h)).astype(bf16),
                x_ref[:, h * HEAD_DIM : (h + 1) * HEAD_DIM],
            )
            for h in range(g * per_group, (g + 1) * per_group)
        ]
        y = carried + jnp.concatenate(within, axis=1)
        y_ref[:, cols] = y
        gated = y * jax.nn.silu(z_ref[:, cols].astype(f32))
        scale = lax.rsqrt(jnp.mean(gated * gated, axis=1, keepdims=True) + epsilon)
        half_ref[:, cols] = (gated * scale).astype(bf16)


def gate_kernel(dn_ref, y_ref, z_ref, c_ref, log_ref, dy_ref, dz_ref, sent_ref):
    length, heads = log_ref.shape
    groups = c_ref.shape[1] // NS
    wide = y_ref.shape[1] // groups
    grown = exact(jnp.exp(cum_logs(log_ref[...])), spread(heads))
    for g in range(groups):
        cols = slice(g * wide, (g + 1) * wide)
        y = y_ref[:, cols]
        z = z_ref[:, cols].astype(f32)
        dn = dn_ref[:, cols]
        sig = jax.nn.sigmoid(z)
        silu = z * sig
        gated = y * silu
        scale = lax.rsqrt(jnp.mean(gated * gated, axis=1, keepdims=True) + epsilon)
        normed = gated * scale
        d_gated = scale * (dn - normed * jnp.mean(dn * normed, axis=1, keepdims=True))
        dy = d_gated * silu
        dy_ref[:, cols] = dy
        dz_ref[:, cols] = (d_gated * y * sig * (1.0 + z * (1.0 - sig))).astype(bf16)
        sent_ref[cols, :] = dot(
            (dy * grown[:, cols]).astype(bf16), c_ref[:, g * NS : (g + 1) * NS], by_rows
        ).astype(bf16)


def within_kernel(
    dy_ref, y_ref, x_ref, b_ref, c_ref, log_ref, entry_ref, dx_ref, db_ref, dc_ref, dl_ref
):
    length, heads = log_ref.shape
    groups = b_ref.shape[1] // NS
    wide = x_ref.shape[1] // groups
    per_group = heads // groups
    log = log_ref[...]
    mask = lower(length)
    cum = cum_logs(log)
    cum_t = exact(log, mask.astype(f32), (((0,), (1,)), ((), ())))
    grown = exact(jnp.exp(cum), spread(heads))
    balance = jnp.zeros((length, heads), f32)
    for g in range(groups):
        cols = slice(g * wide, (g + 1) * wide)
        maps = slice(g * NS, (g + 1) * NS)
        b, c = b_ref[:, maps], c_ref[:, maps]
        scores = dot(c, b, by_cols)
        dy = dy_ref[:, cols]
        dy_half = dy.astype(bf16)
        x = x_ref[:, cols]
        d_scores = jnp.zeros((length, length), f32)
        dx = []
        for k in range(per_group):
            h = g * per_group + k
            part = slice(k * HEAD_DIM, (k + 1) * HEAD_DIM)
            decay = decay_of(cum, cum_t, mask, h)
            d_scores = d_scores + dot(dy_half[:, part], x[:, part], by_cols) * decay
            dx.append(dot((scores * decay).astype(bf16), dy_half[:, part], by_rows))
        dx = jnp.concatenate(dx, axis=1)
        dx_ref[:, cols] = dx
        d_half = d_scores.astype(bf16)
        entry = entry_ref[cols, :].astype(bf16)
        dc_ref[:, maps] = dot(d_half, b) + dot((dy * grown[:, cols]).astype(bf16), entry)
        db_ref[:, maps] = dot(d_half, c, by_rows)
        balance = balance + exact(
            dy * y_ref[:, cols] - x.astype(f32) * dx, spread(heads)[:, cols], by_cols
        )
    dl_ref[...] = balance


def finish_kernel(
    weights_ref, parts_ref, x_ref, b_ref, log_ref, entry_ref, own_ref, dx_ref, db_ref, dl_ref,
    step_ref, map_ref, grad_log_ref, later_ref
):
    length, heads = log_ref.shape
    groups = b_ref.shape[1] // NS
    wide = x_ref.shape[1] // groups
    combine(weights_ref, parts_ref, later_ref)
    cum = cum_logs(log_ref[...])
    last = cum[length - 1 : length, :]
    to_end = exact(jnp.exp(last - cum), spread(heads))
    balance = dl_ref[...]
    crossing = []
    for g in range(groups):
        cols = slice(g * wide, (g + 1) * wide)
        maps = slice(g * NS, (g + 1) * NS)
        later = later_ref[cols, :].astype(bf16)
        x = x_ref[:, cols].astype(f32)
        extra = dot(b_ref[:, maps], later, by_cols) * to_end[:, cols]
        step_ref[:, cols] = (dx_ref[:, cols] + extra).astype(bf16)
        map_ref[:, maps] = db_ref[:, maps] + dot((x * to_end[:, cols]).astype(bf16), later)
        balance = balance - exact(x * extra, spread(heads)[:, cols], by_cols)
    rows = (heads, HEAD_DIM, NS)
    own_sum = jnp.sum((later_ref[...] * own_ref[...]).reshape(rows), axis=1)
    entry_sum = jnp.sum((later_ref[...] * entry_ref[...]).reshape(rows), axis=1)
    ones = jnp.ones((1, NS), f32)
    through = exact(ones, own_sum, by_cols) + jnp.exp(last) * exact(ones, entry_sum, by_cols)
    grad_log_ref[...] = exact(lower(length).astype(f32), balance, by_rows) + through


def call(kernel, outs, *args, scalars=0, scratch=()):
    vmem = pl.BlockSpec(memory_space=pltpu.VMEM)
    smem = pl.BlockSpec(memory_space=pltpu.SMEM)
    return pl.pallas_call(
        kernel,
        out_shape=[jax.ShapeDtypeStruct(*o) for o in outs],
        in_specs=[smem] * scalars + [vmem] * (len(args) - scalars),
        out_specs=[vmem] * len(outs),
        scratch_shapes=list(scratch),
        compiler_params=pltpu.CompilerParams(vmem_limit_bytes=56 * 1024 * 1024),
    )(*args)


def expert_backward(row_block, cot_block, gate_mat, up_mat, down_mat):
    gate_pre = jnp.dot(row_block, gate_mat, preferred_element_type=jnp.float32)
    up_pre = jnp.dot(row_block, up_mat, preferred_element_type=jnp.float32)
    gate_sigmoid = jax.nn.sigmoid(gate_pre)
    hidden = (gate_pre * gate_sigmoid * up_pre).astype(jnp.bfloat16)
    d_act = lax.dot_general(cot_block, down_mat, by_cols, preferred_element_type=jnp.float32)
    d_gate = (d_act * up_pre * gate_sigmoid * (1.0 + gate_pre * (1.0 - gate_sigmoid))).astype(
        jnp.bfloat16
    )
    d_up = (d_act * gate_pre * gate_sigmoid).astype(jnp.bfloat16)
    grad_down = lax.dot_general(hidden, cot_block, by_rows, preferred_element_type=jnp.float32)
    grad_gate = lax.dot_general(row_block, d_gate, by_rows, preferred_element_type=jnp.float32)
    grad_up = lax.dot_general(row_block, d_up, by_rows, preferred_element_type=jnp.float32)
    input_part = lax.dot_general(d_gate, gate_mat, by_cols, preferred_element_type=jnp.float32)
    input_part = input_part + lax.dot_general(
        d_up, up_mat, by_cols, preferred_element_type=jnp.float32
    )
    return (grad_gate, grad_up, grad_down, input_part)


def local(
    hidden_rows,
    out_cot,
    routes,
    route_weight,
    gate_w,
    up_w,
    down_w,
    out_weight,
    step_inputs,
    input_map,
    output_map,
    log_decay,
    gate_z,
):
    wide = step_inputs.shape
    heads = log_decay.shape[1]
    states = (heads * HEAD_DIM, NS)
    place_sp = lax.axis_index("sp")
    sent_state, own_state = call(
        state_kernel,
        [((states[0] + TAIL, NS), bf16), (states, f32)],
        step_inputs, input_map, log_decay,
    )
    state_parts = lax.all_gather(sent_state, "sp")
    totals = jnp.sum(state_parts[:, states[0] : states[0] + 3, :heads].astype(f32), axis=1)
    sources = jnp.arange(lax.axis_size("sp"))
    before = ((sources[None, :] > sources[:, None]) & (sources[None, :] < place_sp)).astype(f32)
    after = ((sources[None, :] < sources[:, None]) & (sources[None, :] > place_sp)).astype(f32)
    entry_weights = jnp.where(
        (sources < place_sp)[:, None], jnp.exp(exact(before, totals)), 0.0
    )
    later_weights = jnp.where(
        (sources > place_sp)[:, None], jnp.exp(exact(after, totals)), 0.0
    )
    entry_state, y, normed_half = call(
        forward_kernel,
        [(states, f32), (wide, f32), (wide, bf16)],
        entry_weights, state_parts, step_inputs, input_map, output_map, log_decay, gate_z,
        scalars=1,
    )
    all_weight = lax.all_gather(out_weight, "sp", axis=0, tiled=True)
    all_half = lax.all_gather(normed_half, "sp", axis=0, tiled=True)
    tok_rows, top_count = routes.shape
    local_experts = gate_w.shape[0]
    sp_devices = lax.axis_size("sp")
    total_experts = local_experts * sp_devices
    capacity = 5 * tok_rows * top_count // (4 * total_experts)
    flat_routes = routes.reshape(-1)
    expert_hits = (
        flat_routes[:, None] == jnp.arange(total_experts, dtype=jnp.int32)[None, :]
    ).astype(jnp.int32)
    slot_rank = jnp.sum((jnp.cumsum(expert_hits, axis=0) - expert_hits) * expert_hits, axis=1)
    target = (flat_routes * capacity + slot_rank).reshape(tok_rows, top_count)
    slot_ids = jnp.arange(total_experts * capacity, dtype=jnp.int32)[:, None]
    matches = [slot_ids == target[:, column][None, :] for column in range(top_count)]
    placing = reduce(jnp.logical_or, matches).astype(jnp.bfloat16)
    slot_weight = reduce(
        jnp.add,
        [
            jnp.sum(jnp.where(matches[column], route_weight[:, column][None, :], 0.0), axis=1)
            for column in range(top_count)
        ],
    )

    def place(source_rows):
        return jnp.dot(placing, source_rows, preferred_element_type=jnp.float32)

    sent_rows = place(hidden_rows).astype(jnp.bfloat16)
    sent_cot = (place(out_cot) * slot_weight[:, None]).astype(jnp.bfloat16)
    part_rows, part_cot = (
        lax.all_to_all(sent_rows, "sp", split_axis=0, concat_axis=0, tiled=True),
        lax.all_to_all(sent_cot, "sp", split_axis=0, concat_axis=0, tiled=True),
    )
    got_rows, got_cot = (
        lax.all_gather(part_rows, "tp", axis=1, tiled=True),
        lax.all_gather(part_cot, "tp", axis=1, tiled=True),
    )
    buffer_rows = sp_devices * capacity
    arranged_rows = (
        got_rows.reshape(sp_devices, local_experts, capacity, D)
        .transpose(1, 0, 2, 3)
        .reshape(local_experts, buffer_rows, D)
    )
    arranged_cot = (
        got_cot.reshape(sp_devices, local_experts, capacity, D)
        .transpose(1, 0, 2, 3)
        .reshape(local_experts, buffer_rows, D)
    )
    grad_gate, grad_up, grad_down, input_part = expert_backward(
        arranged_rows[0], arranged_cot[0], gate_w[0], up_w[0], down_w[0]
    )
    grads_gate = [grad_gate]
    grads_up = [grad_up]
    grads_down = [grad_down]
    partials = [input_part]
    stacked = (
        jnp.stack(partials)
        .reshape(local_experts, sp_devices, capacity, D)
        .transpose(1, 0, 2, 3)
        .reshape(-1, D)
    )
    tp_devices = lax.axis_size("tp")
    pieces = stacked.astype(bf16).reshape(-1, tp_devices, D // tp_devices).transpose(1, 0, 2)
    pieces = lax.all_to_all(pieces, "tp", split_axis=0, concat_axis=0, tiled=True)
    summed = jnp.sum(pieces.astype(f32), axis=0).astype(bf16)
    returned = lax.all_to_all(summed, "sp", split_axis=0, concat_axis=0, tiled=True)
    routed = lax.dot_general(placing, returned, by_rows, preferred_element_type=jnp.float32)
    mid_part = (out_cot.astype(jnp.float32) + routed).astype(jnp.bfloat16)
    mid_grad = lax.all_gather(mid_part, "tp", axis=1, tiled=True)
    mid_cols = lax.all_to_all(mid_grad, "sp", split_axis=1, concat_axis=0, tiled=True)
    d_normed = dot(mid_grad, all_weight)
    dy, grad_gate_z, sent_grad = call(
        gate_kernel,
        [(wide, f32), (wide, bf16), (states, bf16)],
        d_normed, y, gate_z, output_map, log_decay,
    )
    later_parts = lax.all_gather(sent_grad, "sp")
    dx, db, dc, dl = call(
        within_kernel,
        [(wide, f32), (input_map.shape, f32), (output_map.shape, f32), (log_decay.shape, f32)],
        dy, y, step_inputs, input_map, output_map, log_decay, entry_state,
    )
    grad_out_weight = dot(mid_cols, all_half, by_rows)
    grad_step, grad_in_map, grad_log = call(
        finish_kernel,
        [(wide, bf16), (input_map.shape, f32), (log_decay.shape, f32)],
        later_weights, later_parts, step_inputs, input_map, log_decay, entry_state, own_state,
        dx, db, dl,
        scalars=1,
        scratch=[pltpu.VMEM(states, f32)],
    )
    return (
        jnp.stack(grads_gate),
        jnp.stack(grads_up),
        jnp.stack(grads_down),
        grad_out_weight,
        grad_step,
        grad_gate_z,
        grad_in_map,
        dc,
        grad_log,
    )


def solution(mesh):
    placed = (
        P("sp", "tp"),
        P("sp", "tp"),
        P("sp", None),
        P("sp", None),
        P("sp", None, "tp"),
        P("sp", None, "tp"),
        P("sp", "tp", None),
        P("sp", "tp"),
        P("sp", "tp"),
        P("sp", "tp"),
        P("sp", "tp"),
        P("sp", "tp"),
        P("sp", "tp"),
    )
    return jax.shard_map(
        local,
        mesh=mesh,
        in_specs=placed,
        out_specs=(
            P("sp", None, "tp"),
            P("sp", None, "tp"),
            P("sp", "tp", None),
            P("sp", "tp"),
            P("sp", "tp"),
            P("sp", "tp"),
            P("sp", "tp"),
            P("sp", "tp"),
            P("sp", "tp"),
        ),
        check_vma=False,
    )
```
